512 devices in a mesh: gr: 2 (over z_hi), fs: 32 (over z_lo, y), tp: 8 (over x, core).
Axes of the slice: x: 4, y: 4, z: 16 (z_hi: 2, z_lo: 8; z = z_hi * 8 + z_lo), core: 2. Of those that a mesh axis runs over, the one named last changes fastest.
Arguments:
- tokens: bfloat16 [24576, 2048], P(('gr', 'fs')), may hold values from -6 to 6
- route_ids: int32 [24576, 2], P(('gr', 'fs')), may hold values from 0 to 31, as said below
- route_weights: float32 [24576, 2], P(('gr', 'fs')), may hold values from 0.1 to 1
- norm_gain: float32 [2048], P(('gr', 'fs')), may hold values from 0.1 to 1.9
- gate_weight: float32 [32, 2048, 1024], P(None, ('gr', 'fs'), 'tp'), may hold values from -0.125 to 0.125
- up_weight: float32 [32, 2048, 1024], P(None, ('gr', 'fs'), 'tp'), may hold values from -0.125 to 0.125
- down_weight: float32 [32, 1024, 2048], P(None, ('gr', 'fs'), 'tp'), may hold values from -0.1875 to 0.1875
Outputs:
- gate_new: bfloat16 [32, 2048, 1024], P('fs', None, 'tp')
- up_new: bfloat16 [32, 2048, 1024], P('fs', None, 'tp')
- down_new: bfloat16 [32, 1024, 2048], P('fs', 'tp')
- mixed: bfloat16 [24576, 2048], P(('gr', 'fs'), 'tp')
The draws below stay inside these ranges and needn't reach their ends.
Inputs may be any that keep to these rules, and one draw needn't show every extreme that they name: `route_ids`: each row names two different experts of one group (expert e belongs to group e // 8); in each device's block of 384 rows every expert is named by exactly 24 rows.
All inputs are finite; a program needn't handle non-finite values.
Results may differ from the reference program's by a relative error of at most 0.015.
Values may be sent and summed in bfloat16 or wider, within the bound.
A program may use at most 64 MiB of HBM per device.

```python
import jax
import jax.numpy as jnp
from jax import lax

D = 2048
FF = 1024
GROUPS = 4
TOK_DEV = 384
EXPERTS = 32
EPG = 8
HID_DEV = 128
TOKENS = 24576
N_GR = 2
N_FS = 32


def draw_route_ids(key, part):
    blocks = N_GR * N_FS

    def one_block(block_key):
        key_order, key_first, key_step = jax.random.split(block_key, 3)
        place = jax.random.permutation(key_order, TOK_DEV).astype(jnp.int32)
        group = place % GROUPS
        inner = place // GROUPS
        first_shift = jax.random.randint(key_first, (GROUPS,), 0, EPG).astype(jnp.int32)
        step_shift = jax.random.randint(key_step, (GROUPS,), 0, EPG - 1).astype(jnp.int32)
        first = (inner + first_shift[group]) % EPG
        stride = 1 + (inner // EPG + step_shift[group]) % (EPG - 1)
        second = (first + stride) % EPG
        return jnp.stack([group * EPG + first, group * EPG + second], axis=1).astype(jnp.int32)
    keys = jax.random.split(key, blocks)
    return jax.vmap(one_block)(keys).reshape(TOKENS, 2)


def shard_levels(stream_key, shape, cuts, low, top_value):
    gain, own = 1.0, jax.random.fold_in(stream_key, 6)
    for position, shards_of in cuts:
        draws = jnp.exp(jax.random.uniform(jax.random.fold_in(own, position), (shards_of,), jnp.float32, low / len(cuts), top_value / len(cuts)))
        gain = gain * jnp.repeat(draws, shape[position] // shards_of).reshape([-1 if axis == position else 1 for axis in range(len(shape))])
    return gain


def gaussian(own_key, shape, width, limit, cuts=(), held_as=jnp.bfloat16):
    level = shard_levels(own_key, shape, cuts, -0.22, 0.18) if cuts else 1.0
    array = jax.random.normal(own_key, shape, jnp.float32) * width * level
    return jnp.minimum(jnp.maximum(array, -limit), limit).astype(held_as)


def setup_inputs(seed: int = 0) -> dict:
    arg_keys = jax.random.split(jax.random.key(seed), 8)
    return {
        "tokens": gaussian(arg_keys[0], (TOKENS, D), 1.0, 6.0, ((0, 64),)),
        "route_ids": draw_route_ids(jax.random.fold_in(arg_keys[7], 71), 0),
        "route_weights": jnp.clip(0.1 + 0.9 * jax.random.uniform(arg_keys[2], (TOKENS, 2), jnp.float32) ** shard_levels(arg_keys[2], (TOKENS, 2), ((0, 64),), -0.2, 0.2), 0.1, 1.0),
        "norm_gain": jnp.clip(1.0 + 0.18 * jax.random.normal(arg_keys[3], (D,), jnp.float32), 0.1, 1.9),
        "gate_weight": gaussian(arg_keys[4], (EXPERTS, D, FF), D ** -0.5, 0.125, ((1, 64), (2, 8)), jnp.float32),
        "up_weight": gaussian(arg_keys[5], (EXPERTS, D, FF), D ** -0.5, 0.125, ((1, 64), (2, 8)), jnp.float32),
        "down_weight": gaussian(arg_keys[6], (EXPERTS, FF, D), FF ** -0.5, 0.1875, ((1, 64), (2, 8)), jnp.float32),
    }


def expert_block(args):
    gate_one, up_one, down_one, rows = args
    first = jnp.dot(rows, gate_one, preferred_element_type=jnp.float32)
    second = jnp.dot(rows, up_one, preferred_element_type=jnp.float32)
    hidden = (jax.nn.silu(first) * second).astype(jnp.bfloat16)
    count = rows.shape[0]
    pieces = hidden.reshape(count, FF // HID_DEV, HID_DEV).astype(jnp.float32)
    down_pieces = down_one.reshape(FF // HID_DEV, HID_DEV, D).astype(jnp.float32)
    partials = jnp.einsum('mbf,bfd->bmd', pieces, down_pieces).astype(jnp.bfloat16)
    return lax.optimization_barrier(jnp.sum(partials.astype(jnp.float32), axis=0)).astype(jnp.bfloat16)

def reference(tokens, route_ids, route_weights, norm_gain, gate_weight, up_weight, down_weight):
    gate_new = (gate_weight * norm_gain[None, :, None]).astype(jnp.bfloat16)
    up_new = (up_weight * norm_gain[None, :, None]).astype(jnp.bfloat16)
    down_new = down_weight.astype(jnp.bfloat16)
    widened = tokens.astype(jnp.float32)
    normed = (widened * lax.rsqrt(lax.optimization_barrier(jnp.mean(widened * widened, axis=-1, keepdims=True)) + 1e-06)).astype(jnp.bfloat16)
    flat_ids = route_ids.reshape(-1)
    per_expert = flat_ids.shape[0] // EXPERTS
    order = jnp.argsort(flat_ids, stable=True).astype(jnp.int32).reshape(EXPERTS, per_expert)

    def one_expert(args):
        gate_one, up_one, down_one, picks = args
        rows = normed[picks // 2]
        return expert_block((gate_one, up_one, down_one, rows))
    results = lax.map(one_expert, (gate_new, up_new, down_new, order))
    route_out = jnp.zeros((flat_ids.shape[0], D), jnp.bfloat16).at[order.reshape(-1)].set(results.reshape(-1, D))
    route_out = route_out.reshape(-1, 2, D).astype(jnp.float32)
    mixed = lax.optimization_barrier(jnp.sum(route_weights[:, :, None] * route_out, axis=1)).astype(jnp.bfloat16)
    return (gate_new, up_new, down_new, mixed)
```

```python
import jax
import jax.numpy as jnp
from jax import lax
from jax.experimental import pallas as pl
from jax.experimental.pallas import tpu as pltpu
from jax.sharding import Mesh
from jax.sharding import PartitionSpec as P

MESH = pl.DeviceIdType.MESH
BF, F32 = jnp.bfloat16, jnp.float32
NZ, NH, NL, NY, NX, NC = 16, 2, 8, 4, 4, 2
NTP = NX * NC
TOK, WIDTH, CAP, EXP = 384, 2048, 24, 32
WCOL = WIDTH // NTP
ROWS = EXP * CAP


def halves_down(v):
    return jnp.concatenate([v[:, :, :128], v[:, :, 128:]], axis=1)


def kernel(
    tokens, idsc, idsr, wts, gain, gate, up, down,
    gate_out, up_out, down_out, mixed,
    ws, yw, gw, ds, yd, dw, dn, ts, yt, xa, xr, hh, os_, rz, rt, rr, q0, q1,
    y_send, y_recv, z_send, z_recv, x_send, x_recv, b_send, b_recv, c_sem, loc, out_sem,
):
    zh, zl, my = lax.axis_index("zh"), lax.axis_index("zl"), lax.axis_index("y")
    mx, mc = lax.axis_index("x"), lax.axis_index("c")
    zz = zh * NL + zl
    tp = mx * NC + mc

    def at_z(z):
        z = (z + 2 * NZ) % NZ
        return {"zh": z // NL, "zl": z % NL}

    def copy_to(src, dst, send, recv, dev):
        return pltpu.make_async_remote_copy(
            src_ref=src, dst_ref=dst, send_sem=send, recv_sem=recv, device_id=dev, device_id_type=MESH
        )

    def wait_bytes(ref, sem):
        pltpu.make_async_copy(ref, ref, sem).wait()

    bar = pltpu.get_barrier_semaphore()

    @pl.loop(1, NY)
    def _(d):
        pl.semaphore_signal(bar, inc=1, device_id={"y": (my + d) % NY}, device_id_type=MESH)

    @pl.loop(1, NZ)
    def _(d):
        pl.semaphore_signal(bar, inc=1, device_id=at_z(zz + d), device_id_type=MESH)

    @pl.loop(1, NTP)
    def _(d):
        t = (tp + d) % NTP
        pl.semaphore_signal(bar, inc=1, device_id={"x": t // NC, "c": t % NC}, device_id_type=MESH)

    def relabel(e):
        return (e % NY) * NL + e // NY

    first_r, second_r = relabel(idsr[0:1, :]), relabel(idsr[1:2, :])
    ex = lax.broadcasted_iota(jnp.int32, (EXP, TOK), 0)
    member_r = (ex == first_r) | (ex == second_r)
    a = lax.broadcasted_iota(jnp.int32, (TOK, TOK), 0)
    b = lax.broadcasted_iota(jnp.int32, (TOK, TOK), 1)
    before = (a < b).astype(F32).astype(BF)
    rank_r = jnp.dot(member_r.astype(F32).astype(BF), before, preferred_element_type=F32)
    rank_r = jnp.where(member_r, rank_r, -1.0)

    @pl.loop(0, TOK // 64)
    def _(i):
        r = pl.ds(pl.multiple_of(i * 64, 64), 64)
        v = tokens[r, :].astype(F32)
        scale = lax.rsqrt(jnp.mean(v * v, axis=-1, keepdims=True) + 1e-06)
        cols = pl.ds(pl.multiple_of(tp * WCOL, WCOL), WCOL)
        rr[r, :] = (tokens[r, cols].astype(F32) * scale).astype(BF)

    mine = rr[0:TOK, :]
    slot = lax.broadcasted_iota(jnp.int32, (NL, CAP, TOK), 1).astype(F32)
    for yy in range(NY):
        rk = rank_r[yy * NL : (yy + 1) * NL, :]
        pick = jnp.broadcast_to(rk[:, None, :], (NL, CAP, TOK)) == slot
        pick = pick.astype(F32).reshape(NL * CAP, TOK).astype(BF)
        got = jnp.dot(pick, mine, preferred_element_type=F32).reshape(NL, CAP, WCOL)
        ts[yy] = halves_down(got).astype(BF)

    g = jnp.broadcast_to(gain[...], (32, 128))[None, None]
    for yy in range(NY):
        for zt in range(NL):
            e = zt * NY + yy
            ws[yy, zt, :, 0:128] = (gate[e] * g[0, 0]).astype(BF)
            ws[yy, zt, :, 128:256] = (up[e] * g[0, 0]).astype(BF)
            ds[yy, zt] = down[e].astype(BF)

    pl.semaphore_wait(bar, (NY - 1) + (NZ - 1) + (NTP - 1))

    T, W, D = 0, 1, 2
    stage_y = ((ts, yt, T), (ws, yw, W), (ds, yd, D))

    def y_copy(kind, d):
        src, dst, k = stage_y[kind]
        to = (my + d) % NY
        return copy_to(src.at[to], dst.at[my], y_send.at[k, d], y_recv.at[k, d], {"y": to})

    for kind in (T, W, D):
        for d in (1, 3, 2):
            y_copy(kind, d).start()

    def tok_dist(delta):
        if delta < 4:
            return delta
        if delta > 4:
            return delta - NL
        return 4 - NL * (zl % 2)

    def z_tok(src, ys):
        for delta in (4, 3, 5, 2, 6, 1, 7):
            zt = (zl + delta) % NL
            copy_to(
                src.at[zt], xa.at[mx, mc, zl, ys], z_send.at[T], z_recv.at[T], at_z(zz + tok_dist(delta))
            ).start()
        pltpu.make_async_copy(src.at[zl], xa.at[mx, mc, zl, ys], loc.at[T]).start()

    def z_weights(src, into, k, ys):
        def send(far):
            copy_to(src.at[far % NL], into.at[zz, ys], z_send.at[k], z_recv.at[k], at_z(far)).start()

        send(zz + NL)

        @pl.loop(1, NL)
        def _(i):
            send(zz + NL + i)
            send(zz + NL - i)

        pltpu.make_async_copy(src.at[zl], into.at[zz, ys], loc.at[k]).start()

    z_tok(ts.at[my], my)
    z_weights(ws.at[my], gw, W, my)
    for d in (1, 3, 2):
        y_copy(T, d).wait_recv()
        ys = (my + NY - d) % NY
        z_tok(yt.at[ys], ys)
    for d in (1, 3, 2):
        y_copy(W, d).wait_recv()
        ys = (my + NY - d) % NY
        z_weights(yw.at[ys], gw, W, ys)
    z_weights(ds.at[my], dw, D, my)
    for d in (1, 3, 2):
        y_copy(D, d).wait_recv()
        ys = (my + NY - d) % NY
        z_weights(yd.at[ys], dw, D, ys)

    first_c, second_c = relabel(idsc[:, 0:1]), relabel(idsc[:, 1:2])
    exc = lax.broadcasted_iota(jnp.int32, (TOK, EXP), 1)
    is_first, is_second = exc == first_c, exc == second_c
    after = (a > b).astype(F32).astype(BF)
    rank_c = jnp.dot(after, (is_first | is_second).astype(F32).astype(BF), preferred_element_type=F32)
    place = lax.broadcasted_iota(jnp.int32, (TOK, ROWS), 1).astype(F32)
    for is_k, e_k, q in ((is_first, first_c, q0), (is_second, second_c, q1)):
        at = jnp.sum(jnp.where(is_k, rank_c, 0.0), axis=1, keepdims=True) + e_k.astype(F32) * CAP
        q[...] = (place == at).astype(F32).astype(BF)

    wait_bytes(xa.at[0, 0, 0], loc.at[T])
    wait_bytes(xa.at[0, 0, 0:7], z_recv.at[T])

    def x_copy(ref, k, d):
        to = (mx + d) % NX
        return copy_to(ref.at[mx, mc], ref.at[mx, mc], x_send.at[k, d], x_recv.at[k, d], {"x": to})

    def c_copy(ref, k, d):
        who = (mx + NX - d) % NX
        return copy_to(
            ref.at[who, mc], ref.at[who, mc], x_send.at[k, NX + d], x_recv.at[k, NX + d], {"c": 1 - mc}
        )

    def gather_tp(ref, k):
        for d in (1, 3, 2):
            x_copy(ref, k, d).start()
        c_copy(ref, k, 0).start()
        for d in (1, 3, 2):
            x_copy(ref, k, d).wait_recv()
            c_copy(ref, k, d).start()
        for d in range(NX):
            c_copy(ref, k, d).wait_recv()

    gather_tp(xa, 0)

    @pl.loop(0, NL)
    def _(i):
        r = pl.ds(pl.multiple_of(i * NY * CAP, NY * CAP), NY * CAP)
        for x in range(NX):
            for c in range(NC):
                v = xa[x, c, i].astype(F32)
                col = (x * NC + c) * WCOL
                xr[r, col : col + 128] = v[:, :CAP].reshape(NY * CAP, 128).astype(BF)
                xr[r, col + 128 : col + 256] = v[:, CAP:].reshape(NY * CAP, 128).astype(BF)

    wait_bytes(gw.at[0], loc.at[W])
    wait_bytes(gw.at[0:15], z_recv.at[W])
    gate_copy = pltpu.make_async_copy(gw.at[:, :, :, 0:128], gate_out, out_sem.at[0])
    up_copy = pltpu.make_async_copy(gw.at[:, :, :, 128:256], up_out, out_sem.at[1])
    gate_copy.start()
    up_copy.start()
    hid_rows = 128

    @pl.loop(0, ROWS // hid_rows)
    def _(i):
        r = pl.ds(pl.multiple_of(i * hid_rows, hid_rows), hid_rows)
        both = jnp.dot(xr[r, :], gw[...].reshape(WIDTH, 256), preferred_element_type=F32)
        v = both[:, 0:128]
        hh[mx, mc, r, :] = (v / (1.0 + jnp.exp(-v)) * both[:, 128:256]).astype(BF)

    gather_tp(hh, 1)

    wait_bytes(dw.at[0], loc.at[D])
    wait_bytes(dw.at[0:15], z_recv.at[D])

    def tp_copy(d):
        t = (tp + d) % NTP
        return copy_to(
            dw.at[pl.ds(t * 2, 2)], dn.at[tp], x_send.at[2, d], x_recv.at[2, d], {"x": t // NC, "c": t % NC}
        )

    own_dn = pltpu.make_async_copy(dw.at[pl.ds(tp * 2, 2)], dn.at[tp], loc.at[3])

    def back_dist(delta):
        if delta < 4:
            return -delta
        if delta > 4:
            return NL - delta
        return NL * (zl % 2) - 4

    order = (4, 3, 5, 2, 6, 1, 7, 0)

    def back_z(delta):
        src_zl = (zl + NL - delta) % NL
        return copy_to(
            os_.at[src_zl], rz.at[zl], b_send.at[delta], b_recv.at[delta], at_z(zz + back_dist(delta))
        )

    def back_y(delta):
        ex_zl = (zl + delta) % NL
        src = rz.at[ex_zl] if delta else os_.at[zl]
        for d in (2, 1, 3):
            to = (my + d) % NY
            copy_to(src.at[to], rt.at[my, ex_zl], c_sem.at[0], c_sem.at[1], {"y": to}).start()
        pltpu.make_async_copy(src.at[my], rt.at[my, ex_zl], c_sem.at[2]).start()

    for delta in order:
        src_zl = (zl + NL - delta) % NL
        r = pl.ds(pl.multiple_of(src_zl * NY * CAP, NY * CAP), NY * CAP)
        acc = jnp.zeros((NY * CAP, WCOL), F32)
        for x in range(NX):
            lhs = jnp.concatenate([hh[x, 0, r, :], hh[x, 1, r, :]], axis=1)
            acc += jnp.dot(lhs, dw[4 * x : 4 * x + 4].reshape(256, WCOL), preferred_element_type=F32)
        os_[src_zl] = halves_down(acc.reshape(NY, CAP, WCOL)).astype(BF)
        if delta:
            back_z(delta).start()
    back_y(0)
    own_dn.start()
    for d in (1, 7, 2, 6, 3, 5, 4):
        tp_copy(d).start()
    for delta in (1, 7, 2, 6, 3, 5, 4):
        back_z(delta).wait_recv()
        back_y(delta)

    own_dn.wait()
    for d in range(1, NTP):
        tp_copy(d).wait_recv()
    dn_copies = [
        pltpu.make_async_copy(
            dn.at[t].reshape(128, WCOL), down_out.at[:, t * WCOL : (t + 1) * WCOL], out_sem.at[2 + t]
        )
        for t in range(NTP)
    ]
    for copy in dn_copies:
        copy.start()

    wait_bytes(rt.at[0], c_sem.at[2])
    wait_bytes(rt.at[0:3], c_sem.at[1])
    for yy in range(NY):
        v = rt[yy].astype(F32)
        r = slice(yy * NL * CAP, (yy + 1) * NL * CAP)
        rr[r, 0:128] = v[:, :CAP].reshape(NL * CAP, 128).astype(BF)
        rr[r, 128:256] = v[:, CAP:].reshape(NL * CAP, 128).astype(BF)

    for i in range(TOK // 128):
        r = slice(i * 128, (i + 1) * 128)
        one = jnp.dot(q0[r, :], rr[...], preferred_element_type=F32)
        two = jnp.dot(q1[r, :], rr[...], preferred_element_type=F32)
        mixed[r, :] = (wts[r, 0:1] * one + wts[r, 1:2] * two).astype(BF)

    gate_copy.wait()
    up_copy.wait()
    for copy in dn_copies:
        copy.wait()
    for kind in (T, W, D):
        for d in (1, 3, 2):
            y_copy(kind, d).wait_send()
    wait_bytes(xa.at[0, 0, 0:7], z_send.at[T])
    wait_bytes(gw.at[0:15], z_send.at[W])
    wait_bytes(dw.at[0:15], z_send.at[D])
    for ref, k in ((xa, 0), (hh, 1)):
        for d in (1, 3, 2):
            x_copy(ref, k, d).wait_send()
        for d in range(NX):
            c_copy(ref, k, d).wait_send()
    for d in range(1, NTP):
        tp_copy(d).wait_send()
    for delta in range(1, NL):
        back_z(delta).wait_send()
    wait_bytes(rt.at[0:3], c_sem.at[0])


def local(tokens, route_ids, route_weights, norm_gain, gate_weight, up_weight, down_weight):
    vm = pl.BlockSpec(memory_space=pltpu.VMEM)
    far = pl.BlockSpec(memory_space=pl.ANY)
    dma = pltpu.SemaphoreType.DMA
    gate_new, up_new, down_new, mixed = pl.pallas_call(
        kernel,
        out_shape=(
            jax.ShapeDtypeStruct((NZ, NY, 32, 128), BF),
            jax.ShapeDtypeStruct((NZ, NY, 32, 128), BF),
            jax.ShapeDtypeStruct((128, WIDTH), BF),
            jax.ShapeDtypeStruct((TOK, WCOL), BF),
        ),
        in_specs=[vm] * 8,
        out_specs=(far, far, far, vm),
        scratch_shapes=[
            pltpu.VMEM((NY, NL, 32, 256), BF),
            pltpu.VMEM((NY, NL, 32, 256), BF),
            pltpu.VMEM((NZ, NY, 32, 256), BF),
            pltpu.VMEM((NY, NL, 16, WCOL), BF),
            pltpu.VMEM((NY, NL, 16, WCOL), BF),
            pltpu.VMEM((NZ, NY, 16, WCOL), BF),
            pltpu.VMEM((NTP, 2, NY, 16, WCOL), BF),
            pltpu.VMEM((NY, NL, 2 * CAP, 128), BF),
            pltpu.VMEM((NY, NL, 2 * CAP, 128), BF),
            pltpu.VMEM((NX, NC, NL, NY, 2 * CAP, 128), BF),
            pltpu.VMEM((ROWS, WIDTH), BF),
            pltpu.VMEM((NX, NC, ROWS, 128), BF),
            pltpu.VMEM((NL, NY, 2 * CAP, 128), BF),
            pltpu.VMEM((NL, NY, 2 * CAP, 128), BF),
            pltpu.VMEM((NY, NL, 2 * CAP, 128), BF),
            pltpu.VMEM((ROWS, WCOL), BF),
            pltpu.VMEM((TOK, ROWS), BF),
            pltpu.VMEM((TOK, ROWS), BF),
            dma((3, NY)),
            dma((3, NY)),
            dma((3,)),
            dma((3,)),
            dma((3, NTP)),
            dma((3, NTP)),
            dma((NL,)),
            dma((NL,)),
            dma((3,)),
            dma((4,)),
            dma((2 + NTP,)),
        ],
        compiler_params=pltpu.CompilerParams(
            collective_id=0, has_side_effects=True, vmem_limit_bytes=56 * 1024 * 1024
        ),
        name="handoff",
    )(
        tokens,
        route_ids,
        route_ids.T,
        route_weights,
        norm_gain.reshape(32, 1),
        gate_weight,
        up_weight,
        down_weight,
    )
    return (
        gate_new.reshape(1, WIDTH, 128),
        up_new.reshape(1, WIDTH, 128),
        down_new.reshape(1, 128, WIDTH),
        mixed,
    )


def solution(mesh):
    torus = Mesh(mesh.devices.reshape(NH, NL, NY, NX, NC), ("zh", "zl", "y", "x", "c"))
    rows, cols = ("zh", "zl", "y"), ("x", "c")
    placed = (P(rows, None),) * 3 + (P(rows),) + (P(None, rows, cols),) * 3
    experts = ("zl", "y")
    return jax.shard_map(
        local,
        mesh=torus,
        in_specs=placed,
        out_specs=(P(experts, None, cols), P(experts, None, cols), P(experts, cols, None), P(rows, cols)),
        check_vma=False,
    )
```

```python
import jax
import jax.numpy as jnp
from jax import lax
from jax.experimental import pallas as pl
from jax.experimental.pallas import tpu as pltpu
from jax.sharding import Mesh
from jax.sharding import PartitionSpec as P

MESH = pl.DeviceIdType.MESH
BF, F32 = jnp.bfloat16, jnp.float32
NZ, NH, NL, NY, NX, NC = 16, 2, 8, 4, 4, 2
NTP = NX * NC
TOK, WIDTH, CAP, EXP = 384, 2048, 24, 32
WCOL = WIDTH // NTP
ROWS = EXP * CAP
VMEM_MOVE, VMEM_LAST = 57, 57


def halves_down(v):
    return jnp.concatenate([v[:, :, :128], v[:, :, 128:]], axis=1)


def kernel(
    tokens_in, ids_in, wts_in, gain_in, gate_in, up_in, down_in,
    gw_out, dn, rt, cols_out,
    tokens, ids, wts, gain, gate, up, down, ws, yw, gw, ds, yd, dw, ts, yt, xa, xr, hh, os_, rr, cols,
    y_send, y_recv, z_send, z_recv, x_send, x_recv, b_send, b_recv, loc, in_sem, out_sem,
):
    zh, zl, my = lax.axis_index("zh"), lax.axis_index("zl"), lax.axis_index("y")
    mx, mc = lax.axis_index("x"), lax.axis_index("c")
    zz = zh * NL + zl
    tp = mx * NC + mc

    def at_z(z):
        z = (z + 2 * NZ) % NZ
        return {"zh": z // NL, "zl": z % NL}

    def copy_to(src, dst, send, recv, dev):
        return pltpu.make_async_remote_copy(
            src_ref=src, dst_ref=dst, send_sem=send, recv_sem=recv, device_id=dev, device_id_type=MESH
        )

    def wait_bytes(ref, sem):
        pltpu.make_async_copy(ref, ref, sem).wait()

    bar = pltpu.get_barrier_semaphore()

    def greet(dev):
        pl.semaphore_signal(bar, inc=1, device_id=dev, device_id_type=MESH)

    greet(at_z(zz + NL))

    @pl.loop(1, NL)
    def _(d):
        greet(at_z(zz + NL + d))
        greet(at_z(zz + NL - d))

    ins = [
        pltpu.make_async_copy(far, near, in_sem.at[i])
        for i, (far, near) in enumerate(
            (
                (gate_in, gate), (up_in, up), (gain_in, gain), (tokens_in, tokens), (ids_in, ids), (wts_in, wts),
                (down_in, down),
            )
        )
    ]
    for copy in ins:
        copy.start()

    @pl.loop(1, NY)
    def _(d):
        greet({"y": (my + d) % NY})

    @pl.loop(1, NTP)
    def _(d):
        t = (tp + d) % NTP
        greet({"x": t // NC, "c": t % NC})

    with jax.named_scope("w_gain"):
        ins[2].wait()
        eye = lax.broadcasted_iota(jnp.int32, (32, 32), 0) == lax.broadcasted_iota(jnp.int32, (32, 32), 1)
    g = jnp.sum(jnp.where(eye, jnp.broadcast_to(gain[...], (32, 32)), 0.0), axis=1, keepdims=True)
    g = jnp.broadcast_to(g, (32, 128))
    with jax.named_scope("fold"):
        ins[0].wait()
        ins[1].wait()
        for yy in range(NY):
            for zt in range(NL):
                e = zt * NY + yy
                ws[yy, zt, :, 0:128] = (gate[e] * g).astype(BF)
                ws[yy, zt, :, 128:256] = (up[e] * g).astype(BF)

    with jax.named_scope("w_bar"):
        pl.semaphore_wait(bar, (NY - 1) + (NZ - 1) + (NTP - 1))

    T, W, D = 0, 1, 2

    def y_copy(k, d):
        to = (my + d) % NY
        src, dst = (
            (ts.at[to], yt.at[my]) if k == T else (ws.at[to], yw.at[my]) if k == W else (ds.at[:, to], yd.at[:, my])
        )
        return copy_to(src, dst, y_send.at[k, d], y_recv.at[k, d], {"y": to})

    def tok_dist(delta):
        if delta < 4:
            return delta
        if delta > 4:
            return delta - NL
        return 4 - NL * (zl % 2)

    def z_tok(src, ys):
        for delta in (4, 3, 5, 2, 6, 1, 7):
            zt = (zl + delta) % NL
            copy_to(
                src.at[zt], xa.at[mx, mc, zl, ys], z_send.at[T], z_recv.at[T], at_z(zz + tok_dist(delta))
            ).start()
        pltpu.make_async_copy(src.at[zl], xa.at[mx, mc, zl, ys], loc.at[T]).start()

    def z_weights(src, into, k, ys):
        def send(far):
            copy_to(src.at[far % NL], into.at[zz, ys], z_send.at[k], z_recv.at[k], at_z(far)).start()

        send(zz + NL)

        @pl.loop(1, NL)
        def _(i):
            send(zz + NL + i)
            send(zz + NL - i)

        pltpu.make_async_copy(src.at[zl], into.at[zz, ys], loc.at[k]).start()

    def z_down(h):
        def send(far):
            copy_to(yd.at[h, :, far % NL], dw.at[h, zz], z_send.at[D + h], z_recv.at[D + h], at_z(far)).start()

        send(zz + NL)
        pltpu.make_async_copy(yd.at[h, :, zl], dw.at[h, zz], loc.at[D + h]).start()

        @pl.loop(1, NL)
        def _(i):
            send(zz + NL + i)
            send(zz + NL - i)

    with jax.named_scope("send_w"):
        for d in (1, 3, 2):
            y_copy(W, d).start()
        z_weights(ws.at[my], gw, W, my)

    def relabel(e):
        return (e % NY) * NL + e // NY

    ins[4].wait()
    ins[5].wait()
    first_r, second_r = relabel(ids[0:1, :]), relabel(ids[1:2, :])
    ex = lax.broadcasted_iota(jnp.int32, (EXP, TOK), 0)
    member_r = (ex == first_r) | (ex == second_r)
    a = lax.broadcasted_iota(jnp.int32, (TOK, TOK), 0)
    b = lax.broadcasted_iota(jnp.int32, (TOK, TOK), 1)
    before = (a < b).astype(F32).astype(BF)
    rank_r = jnp.dot(member_r.astype(F32).astype(BF), before, preferred_element_type=F32)
    rank_r = jnp.where(member_r, rank_r, -1.0)

    ins[3].wait()

    @pl.loop(0, TOK // 64)
    def _(i):
        r = pl.ds(pl.multiple_of(i * 64, 64), 64)
        v = tokens[r, :].astype(F32)
        scale = lax.rsqrt(jnp.mean(v * v, axis=-1, keepdims=True) + 1e-06)
        own = pl.ds(pl.multiple_of(tp * WCOL, WCOL), WCOL)
        rr[r, :] = (tokens[r, own].astype(F32) * scale).astype(BF)

    mine = rr[0:TOK, :]
    slot = lax.broadcasted_iota(jnp.int32, (NL, CAP, TOK), 1).astype(F32)
    for yy in range(NY):
        rk = rank_r[yy * NL : (yy + 1) * NL, :]
        pick = jnp.broadcast_to(rk[:, None, :], (NL, CAP, TOK)) == slot
        pick = pick.astype(F32).reshape(NL * CAP, TOK).astype(BF)
        got = jnp.dot(pick, mine, preferred_element_type=F32).reshape(NL, CAP, WCOL)
        ts[yy] = halves_down(got).astype(BF)

    with jax.named_scope("send_t"):
        for d in (1, 3, 2):
            y_copy(T, d).start()
        z_tok(ts.at[my], my)

    ins[6].wait()
    for yy in range(NY):
        for zt in range(NL):
            both = down[zt * NY + yy].astype(BF)
            ds[0, yy, zt] = both[:, 0:128]
            ds[1, yy, zt] = both[:, 128:256]

    for d in (1, 3, 2):
        y_copy(D, d).start()
    own_down = pltpu.make_async_copy(ds.at[:, my], yd.at[:, my], loc.at[4])
    own_down.start()
    with jax.named_scope("fwd_t"):
        for d in (1, 3, 2):
            y_copy(T, d).wait_recv()
            ys = (my + NY - d) % NY
            z_tok(yt.at[ys], ys)
    with jax.named_scope("fwd_w"):
        for d in (1, 3, 2):
            y_copy(W, d).wait_recv()
            ys = (my + NY - d) % NY
            z_weights(yw.at[ys], gw, W, ys)
    with jax.named_scope("fwd_d"):
        for d in (1, 3, 2):
            y_copy(D, d).wait_recv()
        own_down.wait()
        z_down(0)
        z_down(1)

    ats = [
        jnp.sum(jnp.where(ex == e_k, rank_r, 0.0), axis=0, keepdims=True) + e_k.astype(F32) * CAP
        for e_k in (first_r, second_r)
    ]
    turned = jnp.concatenate([*ats, wts[...], jnp.zeros((4, TOK), F32)], axis=0).T
    cols[...] = jnp.concatenate([turned, jnp.zeros((TOK, 120), F32)], axis=1)
    outs = [
        pltpu.make_async_copy(near, far, out_sem.at[i])
        for i, (near, far) in enumerate(((cols, cols_out), (gw, gw_out)))
    ]
    outs[0].start()

    with jax.named_scope("w_ztok"):
        wait_bytes(xa.at[0, 0, 0], loc.at[T])
        wait_bytes(xa.at[0, 0, 0:7], z_recv.at[T])

    def x_copy(ref, k, d):
        to = (mx + d) % NX
        return copy_to(ref.at[mx, mc], ref.at[mx, mc], x_send.at[k, d], x_recv.at[k, d], {"x": to})

    def c_copy(ref, k, d):
        who = (mx + NX - d) % NX
        return copy_to(
            ref.at[who, mc], ref.at[who, mc], x_send.at[k, NX + d], x_recv.at[k, NX + d], {"c": 1 - mc}
        )

    def gather_tp(ref, k):
        for d in (1, 3, 2):
            x_copy(ref, k, d).start()
        c_copy(ref, k, 0).start()
        for d in (1, 3, 2):
            x_copy(ref, k, d).wait_recv()
            c_copy(ref, k, d).start()
        for d in range(NX):
            c_copy(ref, k, d).wait_recv()

    with jax.named_scope("gather_x"):
        gather_tp(xa, 0)

    @pl.loop(0, NL)
    def _(i):
        r = pl.ds(pl.multiple_of(i * NY * CAP, NY * CAP), NY * CAP)
        for x in range(NX):
            for c in range(NC):
                v = xa[x, c, i].astype(F32)
                col = (x * NC + c) * WCOL
                xr[r, col : col + 128] = v[:, :CAP].reshape(NY * CAP, 128).astype(BF)
                xr[r, col + 128 : col + 256] = v[:, CAP:].reshape(NY * CAP, 128).astype(BF)

    with jax.named_scope("w_zw"):
        wait_bytes(gw.at[0], loc.at[W])
        wait_bytes(gw.at[0:15], z_recv.at[W])
    outs[1].start()
    hid_rows = 128

    @pl.loop(0, ROWS // hid_rows)
    def _(i):
        r = pl.ds(pl.multiple_of(i * hid_rows, hid_rows), hid_rows)
        both = jnp.dot(xr[r, :], gw[...].reshape(WIDTH, 256), preferred_element_type=F32)
        v = both[:, 0:128]
        hh[mx, mc, r, :] = (v / (1.0 + jnp.exp(-v)) * both[:, 128:256]).astype(BF)

    with jax.named_scope("gather_h"):
        gather_tp(hh, 1)

    def back_dist(delta):
        if delta < 4:
            return -delta
        if delta > 4:
            return NL - delta
        return NL * (zl % 2) - 4


    def tp_copy(h, d):
        t = (tp + d) % NTP
        return copy_to(
            dw.at[h, pl.ds(t * 2, 2)], dn.at[tp, h], x_send.at[2 + h, d], x_recv.at[2 + h, d],
            {"x": t // NC, "c": t % NC},
        )

    def own_dn(h):
        return pltpu.make_async_copy(dw.at[h, pl.ds(tp * 2, 2)], dn.at[tp, h], loc.at[5 + h])

    def back(h, delta, ys):
        return copy_to(
            os_.at[h, (zl + NL - delta) % NL, ys], rt.at[h, my, zl], b_send.at[h, min(delta, 1)], b_recv.at[h],
            {**at_z(zz + back_dist(delta)), "y": ys},
        )

    def back_own(h):
        return pltpu.make_async_copy(os_.at[h, zl, my], rt.at[h, my, zl], b_recv.at[h])

    def give_back(h):
        with jax.named_scope("w_zd"):
            wait_bytes(dw.at[h, 0], loc.at[D + h])
            wait_bytes(dw.at[h, 0:15], z_recv.at[D + h])
        for delta in (4, 3, 5, 2, 6, 1, 7, 0):
            src_zl = (zl + NL - delta) % NL
            r = pl.ds(pl.multiple_of(src_zl * NY * CAP, NY * CAP), NY * CAP)
            acc = jnp.zeros((NY * CAP, 128), F32)
            for x in range(NX):
                lhs = jnp.concatenate([hh[x, 0, r, :], hh[x, 1, r, :]], axis=1)
                acc += jnp.dot(lhs, dw[h, 4 * x : 4 * x + 4].reshape(256, 128), preferred_element_type=F32)
            os_[h, src_zl] = acc.reshape(NY, 3, 8, 128).astype(BF)
            for d in range(NY):
                if delta or d:
                    back(h, delta, (my + d) % NY).start()
        back_own(h).start()
        own_dn(h).start()
        for d in (1, 7, 2, 6, 3, 5, 4):
            tp_copy(h, d).start()

    with jax.named_scope("give0"):
        give_back(0)
    with jax.named_scope("give1"):
        give_back(1)
    with jax.named_scope("w_back"):
        for h in range(2):
            wait_bytes(rt.at[h], b_recv.at[h])

    with jax.named_scope("drain"):
        for h in range(2):
            own_dn(h).wait()
            for d in range(1, NTP):
                tp_copy(h, d).wait()
            wait_bytes(dw.at[h, 0:15], z_send.at[D + h])
            wait_bytes(os_.at[h, 0, 0:3], b_send.at[h, 0])
            wait_bytes(os_.at[h, 0:7], b_send.at[h, 1])
        for copy in outs:
            copy.wait()
        for kind in (T, W, D):
            for d in (1, 3, 2):
                y_copy(kind, d).wait_send()
        wait_bytes(xa.at[0, 0, 0:7], z_send.at[T])
        wait_bytes(gw.at[0:15], z_send.at[W])
        for ref, k in ((xa, 0), (hh, 1)):
            for d in (1, 3, 2):
                x_copy(ref, k, d).wait_send()
            for d in range(NX):
                c_copy(ref, k, d).wait_send()


def finish(
    gw_in, dn_in, rt_in, cols_in, gate_out, up_out, down_out, mixed_out, gw, dn, rt, cols, rr, mixed, in_sem, sem
):
    ins = [
        pltpu.make_async_copy(far, near, in_sem.at[i])
        for i, (far, near) in enumerate(((cols_in, cols), (rt_in, rt), (gw_in, gw), (dn_in, dn)))
    ]
    for copy in ins:
        copy.start()
    place = lax.broadcasted_iota(jnp.int32, (TOK, ROWS), 1).astype(F32)
    ins[0].wait()
    q0 = (place == cols[:, 0:1]).astype(F32).astype(BF)
    q1 = (place == cols[:, 1:2]).astype(F32).astype(BF)

    ins[1].wait()
    for h in range(2):
        for yy in range(NY):
            r = slice(yy * NL * CAP, (yy + 1) * NL * CAP)
            rr[r, h * 128 : h * 128 + 128] = rt[h, yy].astype(F32).reshape(NL * CAP, 128).astype(BF)
    copies = []

    def put(near, far):
        copies.append(pltpu.make_async_copy(near, far, sem.at[len(copies)]))
        copies[-1].start()

    ins[2].wait()
    put(gw.at[:, :, :, 0:128], gate_out)
    put(gw.at[:, :, :, 128:256], up_out)
    ins[3].wait()
    for t in range(NTP):
        for h in range(2):
            at = t * WCOL + h * 128
            put(dn.at[t, h], down_out.at[:, :, :, at : at + 128])
    for i in range(TOK // 128):
        r = slice(i * 128, (i + 1) * 128)
        one = jnp.dot(q0[r, :], rr[...], preferred_element_type=F32)
        two = jnp.dot(q1[r, :], rr[...], preferred_element_type=F32)
        mixed[r, :] = (cols[r, 2:3] * one + cols[r, 3:4] * two).astype(BF)
        put(mixed.at[r], mixed_out.at[r])
    for copy in copies:
        copy.wait()


def local(tokens, route_ids, route_weights, norm_gain, gate_weight, up_weight, down_weight):
    hbm = pl.BlockSpec(memory_space=pltpu.HBM)
    free = pl.BlockSpec(memory_space=pl.ANY)
    dma = pltpu.SemaphoreType.DMA
    moved = pl.pallas_call(
        kernel,
        out_shape=(
            jax.ShapeDtypeStruct((NZ, NY, 32, 256), BF),
            jax.ShapeDtypeStruct((NTP, 2, 2, NY, 16, 128), BF),
            jax.ShapeDtypeStruct((2, NY, NL, 3, 8, 128), BF),
            jax.ShapeDtypeStruct((TOK, 128), F32),
        ),
        in_specs=[hbm] * 7,
        out_specs=(free,) * 4,
        scratch_shapes=[
            pltpu.VMEM((TOK, WIDTH), BF),
            pltpu.VMEM((2, TOK), jnp.int32),
            pltpu.VMEM((2, TOK), F32),
            pltpu.VMEM((1, 32), F32),
            pltpu.VMEM((EXP, 32, 128), F32),
            pltpu.VMEM((EXP, 32, 128), F32),
            pltpu.VMEM((EXP, 16, WCOL), F32),
            pltpu.VMEM((NY, NL, 32, 256), BF),
            pltpu.VMEM((NY, NL, 32, 256), BF),
            pltpu.VMEM((NZ, NY, 32, 256), BF),
            pltpu.VMEM((2, NY, NL, 16, 128), BF),
            pltpu.VMEM((2, NY, NL, 16, 128), BF),
            pltpu.VMEM((2, NZ, NY, 16, 128), BF),
            pltpu.VMEM((NY, NL, 2 * CAP, 128), BF),
            pltpu.VMEM((NY, NL, 2 * CAP, 128), BF),
            pltpu.VMEM((NX, NC, NL, NY, 2 * CAP, 128), BF),
            pltpu.VMEM((ROWS, WIDTH), BF),
            pltpu.VMEM((NX, NC, ROWS, 128), BF),
            pltpu.VMEM((2, NL, NY, 3, 8, 128), BF),
            pltpu.VMEM((TOK, WCOL), BF),
            pltpu.VMEM((TOK, 128), F32),
            dma((3, NY)),
            dma((3, NY)),
            dma((4,)),
            dma((4,)),
            dma((4, NTP)),
            dma((4, NTP)),
            dma((2, 2)),
            dma((2,)),
            dma((7,)),
            dma((7,)),
            dma((2,)),
        ],
        compiler_params=pltpu.CompilerParams(
            collective_id=0, has_side_effects=True, vmem_limit_bytes=VMEM_MOVE * 1024 * 1024
        ),
        name="handoff",
    )(
        tokens,
        route_ids.T,
        route_weights.T,
        norm_gain.reshape(1, 32),
        gate_weight,
        up_weight,
        down_weight,
    )
    gate_new, up_new, down_new, mixed = pl.pallas_call(
        finish,
        out_shape=(
            jax.ShapeDtypeStruct((NZ, NY, 32, 128), BF),
            jax.ShapeDtypeStruct((NZ, NY, 32, 128), BF),
            jax.ShapeDtypeStruct((2, NY, 16, WIDTH), BF),
            jax.ShapeDtypeStruct((TOK, WCOL), BF),
        ),
        in_specs=[hbm] * 4,
        out_specs=(hbm,) * 4,
        scratch_shapes=[
            pltpu.VMEM((NZ, NY, 32, 256), BF),
            pltpu.VMEM((NTP, 2, 2, NY, 16, 128), BF),
            pltpu.VMEM((2, NY, NL, 3, 8, 128), BF),
            pltpu.VMEM((TOK, 128), F32),
            pltpu.VMEM((ROWS, WCOL), BF),
            pltpu.VMEM((TOK, WCOL), BF),
            dma((4,)),
            dma((2 + 2 * NTP + TOK // 128,)),
        ],
        compiler_params=pltpu.CompilerParams(vmem_limit_bytes=VMEM_LAST * 1024 * 1024),
        name="finish",
    )(*moved)
    return (
        gate_new.reshape(1, WIDTH, 128),
        up_new.reshape(1, WIDTH, 128),
        down_new.reshape(1, 128, WIDTH),
        mixed,
    )


def solution(mesh):
    torus = Mesh(mesh.devices.reshape(NH, NL, NY, NX, NC), ("zh", "zl", "y", "x", "c"))
    rows, cols = ("zh", "zl", "y"), ("x", "c")
    placed = (P(rows, None),) * 3 + (P(rows),) + (P(None, rows, cols),) * 3
    experts = ("zl", "y")
    return jax.shard_map(
        local,
        mesh=torus,
        in_specs=placed,
        out_specs=(P(experts, None, cols), P(experts, None, cols), P(experts, cols, None), P(rows, cols)),
        check_vma=False,
    )
```

```python
import jax
import jax.numpy as jnp
from jax import lax
from jax.experimental import pallas as pl
from jax.experimental.pallas import tpu as pltpu
from jax.sharding import Mesh
from jax.sharding import PartitionSpec as P

MESH = pl.DeviceIdType.MESH
BF, F32 = jnp.bfloat16, jnp.float32
NZ, NH, NL, NY, NX, NC = 16, 2, 8, 4, 4, 2
NTP = NX * NC
TOK, WIDTH, CAP, EXP = 384, 2048, 24, 32
WCOL = WIDTH // NTP
ROWS = EXP * CAP
NEAR = 4
VMEM_MOVE, VMEM_LAST = 57, 57


def halves_down(v):
    return jnp.concatenate([v[:, :, :128], v[:, :, 128:]], axis=1)


def kernel(
    tokens_in, ids_in, wts_in, gain_in, gate_in, up_in, down_in,
    gw_out, dn, rt, cols_out,
    tokens, ids, wts, gain, gate, up, down, ws, yw, gw, ds, yd, dw, ts, yt, xa, xr, hh, os_, rr, cols,
    y_send, y_recv, z_send, z_recv, x_send, x_recv, b_send, b_recv, loc, in_sem, out_sem, far_in,
):
    zh, zl, my = lax.axis_index("zh"), lax.axis_index("zl"), lax.axis_index("y")
    mx, mc = lax.axis_index("x"), lax.axis_index("c")
    zz = zh * NL + zl
    tp = mx * NC + mc

    def at_z(z):
        z = (z + 2 * NZ) % NZ
        return {"zh": z // NL, "zl": z % NL}

    def copy_to(src, dst, send, recv, dev):
        return pltpu.make_async_remote_copy(
            src_ref=src, dst_ref=dst, send_sem=send, recv_sem=recv, device_id=dev, device_id_type=MESH
        )

    def wait_bytes(ref, sem):
        pltpu.make_async_copy(ref, ref, sem).wait()

    bar = pltpu.get_barrier_semaphore()

    def greet(dev):
        pl.semaphore_signal(bar, inc=1, device_id=dev, device_id_type=MESH)

    @pl.loop(0, NEAR)
    def _(i):
        greet(at_z(zz + NEAR - i))
        greet(at_z(zz + NZ - NEAR + i))

    ins = [
        pltpu.make_async_copy(far, near, in_sem.at[i])
        for i, (far, near) in enumerate(
            (
                (gate_in, gate), (up_in, up), (gain_in, gain), (tokens_in, tokens), (ids_in, ids), (wts_in, wts),
                (down_in, down),
            )
        )
    ]
    for copy in ins:
        copy.start()

    @pl.loop(1, NY)
    def _(d):
        greet({"y": (my + d) % NY})

    @pl.loop(1, NTP)
    def _(d):
        t = (tp + d) % NTP
        greet({"x": t // NC, "c": t % NC})

    with jax.named_scope("w_gain"):
        ins[2].wait()
        eye = lax.broadcasted_iota(jnp.int32, (32, 32), 0) == lax.broadcasted_iota(jnp.int32, (32, 32), 1)
    g = jnp.sum(jnp.where(eye, jnp.broadcast_to(gain[...], (32, 32)), 0.0), axis=1, keepdims=True)
    g = jnp.broadcast_to(g, (32, 128))
    with jax.named_scope("fold"):
        ins[0].wait()
        ins[1].wait()
        for yy in range(NY):
            for zt in range(NL):
                e = zt * NY + yy
                ws[yy, zt, :, 0:128] = (gate[e] * g).astype(BF)
                ws[yy, zt, :, 128:256] = (up[e] * g).astype(BF)

    with jax.named_scope("w_bar"):
        pl.semaphore_wait(bar, (NY - 1) + 2 * NEAR + (NTP - 1))
    for i, z in enumerate((zz + NEAR, zz + NZ - NEAR)):
        pl.semaphore_signal(far_in.at[i], inc=1, device_id=at_z(z), device_id_type=MESH)

    T, W, D = 0, 1, 2

    def y_copy(k, d):
        to = (my + d) % NY
        src, dst = (
            (ts.at[to], yt.at[my]) if k == T else (ws.at[to], yw.at[my]) if k == W else (ds.at[:, to], yd.at[:, my])
        )
        return copy_to(src, dst, y_send.at[k, d], y_recv.at[k, d], {"y": to})

    def tok_dist(delta):
        if delta < 4:
            return delta
        if delta > 4:
            return delta - NL
        return 4 - NL * (zl % 2)

    def z_tok(src, ys):
        for delta in (4, 3, 5, 2, 6, 1, 7):
            zt = (zl + delta) % NL
            copy_to(
                src.at[zt], xa.at[mx, mc, zl, ys], z_send.at[T], z_recv.at[T], at_z(zz + tok_dist(delta))
            ).start()
        pltpu.make_async_copy(src.at[zl], xa.at[mx, mc, zl, ys], loc.at[T]).start()

    def z_weights(src, into, k, ys):
        def send(far):
            copy_to(src.at[far % NL], into.at[zz, ys], z_send.at[k], z_recv.at[k], at_z(far)).start()

        send(zz + NL)

        @pl.loop(1, NL)
        def _(i):
            send(zz + NL + i)
            send(zz + NL - i)

        pltpu.make_async_copy(src.at[zl], into.at[zz, ys], loc.at[k]).start()

    def z_down(h):
        def send(far):
            copy_to(yd.at[h, :, far % NL], dw.at[h, zz], z_send.at[D + h], z_recv.at[D + h], at_z(far)).start()

        send(zz + NL)
        pltpu.make_async_copy(yd.at[h, :, zl], dw.at[h, zz], loc.at[D + h]).start()

        @pl.loop(1, NL)
        def _(i):
            send(zz + NL + i)
            send(zz + NL - i)

    def own_w(far):
        copy_to(ws.at[my, far % NL], gw.at[zz, my], z_send.at[W], z_recv.at[W], at_z(far)).start()

    with jax.named_scope("send_w"):
        for d in (1, 3, 2):
            y_copy(W, d).start()
        pltpu.make_async_copy(ws.at[my, zl], gw.at[zz, my], loc.at[W]).start()

        @pl.loop(0, NEAR)
        def _(i):
            own_w(zz + NEAR - i)
            own_w(zz + NZ - NEAR + i)

    def relabel(e):
        return (e % NY) * NL + e // NY

    ins[4].wait()
    ins[5].wait()
    first_r, second_r = relabel(ids[0:1, :]), relabel(ids[1:2, :])
    ex = lax.broadcasted_iota(jnp.int32, (EXP, TOK), 0)
    member_r = (ex == first_r) | (ex == second_r)
    a = lax.broadcasted_iota(jnp.int32, (TOK, TOK), 0)
    b = lax.broadcasted_iota(jnp.int32, (TOK, TOK), 1)
    before = (a < b).astype(F32).astype(BF)
    rank_r = jnp.dot(member_r.astype(F32).astype(BF), before, preferred_element_type=F32)
    rank_r = jnp.where(member_r, rank_r, -1.0)

    ins[3].wait()

    @pl.loop(0, TOK // 64)
    def _(i):
        r = pl.ds(pl.multiple_of(i * 64, 64), 64)
        v = tokens[r, :].astype(F32)
        scale = lax.rsqrt(jnp.mean(v * v, axis=-1, keepdims=True) + 1e-06)
        own = pl.ds(pl.multiple_of(tp * WCOL, WCOL), WCOL)
        rr[r, :] = (tokens[r, own].astype(F32) * scale).astype(BF)

    mine = rr[0:TOK, :]
    slot = lax.broadcasted_iota(jnp.int32, (NL, CAP, TOK), 1).astype(F32)
    for yy in range(NY):
        rk = rank_r[yy * NL : (yy + 1) * NL, :]
        pick = jnp.broadcast_to(rk[:, None, :], (NL, CAP, TOK)) == slot
        pick = pick.astype(F32).reshape(NL * CAP, TOK).astype(BF)
        got = jnp.dot(pick, mine, preferred_element_type=F32).reshape(NL, CAP, WCOL)
        ts[yy] = halves_down(got).astype(BF)

    with jax.named_scope("send_t"):
        for d in (1, 3, 2):
            y_copy(T, d).start()
        z_tok(ts.at[my], my)

    with jax.named_scope("w_far"):
        pl.semaphore_wait(far_in.at[0], 1)
        pl.semaphore_wait(far_in.at[1], 1)
        own_w(zz + NL)

        @pl.loop(1, NL - NEAR)
        def _(i):
            own_w(zz + NL + i)
            own_w(zz + NL - i)

    ins[6].wait()
    for yy in range(NY):
        for zt in range(NL):
            both = down[zt * NY + yy].astype(BF)
            ds[0, yy, zt] = both[:, 0:128]
            ds[1, yy, zt] = both[:, 128:256]

    for d in (1, 3, 2):
        y_copy(D, d).start()
    own_down = pltpu.make_async_copy(ds.at[:, my], yd.at[:, my], loc.at[4])
    own_down.start()
    with jax.named_scope("fwd_t"):
        for d in (1, 3, 2):
            y_copy(T, d).wait_recv()
            ys = (my + NY - d) % NY
            z_tok(yt.at[ys], ys)
    with jax.named_scope("fwd_w"):
        for d in (1, 3, 2):
            y_copy(W, d).wait_recv()
            ys = (my + NY - d) % NY
            z_weights(yw.at[ys], gw, W, ys)
    with jax.named_scope("fwd_d"):
        for d in (1, 3, 2):
            y_copy(D, d).wait_recv()
        own_down.wait()
        z_down(0)
        z_down(1)

    ats = [
        jnp.sum(jnp.where(ex == e_k, rank_r, 0.0), axis=0, keepdims=True) + e_k.astype(F32) * CAP
        for e_k in (first_r, second_r)
    ]
    turned = jnp.concatenate([*ats, wts[...], jnp.zeros((4, TOK), F32)], axis=0).T
    cols[...] = jnp.concatenate([turned, jnp.zeros((TOK, 120), F32)], axis=1)
    outs = [
        pltpu.make_async_copy(near, far, out_sem.at[i])
        for i, (near, far) in enumerate(((cols, cols_out), (gw, gw_out)))
    ]
    outs[0].start()

    with jax.named_scope("w_ztok"):
        wait_bytes(xa.at[0, 0, 0], loc.at[T])
        wait_bytes(xa.at[0, 0, 0:7], z_recv.at[T])

    def x_copy(ref, k, d):
        to = (mx + d) % NX
        return copy_to(ref.at[mx, mc], ref.at[mx, mc], x_send.at[k, d], x_recv.at[k, d], {"x": to})

    def c_copy(ref, k, d):
        who = (mx + NX - d) % NX
        return copy_to(
            ref.at[who, mc], ref.at[who, mc], x_send.at[k, NX + d], x_recv.at[k, NX + d], {"c": 1 - mc}
        )

    def gather_tp(ref, k):
        for d in (1, 3, 2):
            x_copy(ref, k, d).start()
        c_copy(ref, k, 0).start()
        for d in (1, 3, 2):
            x_copy(ref, k, d).wait_recv()
            c_copy(ref, k, d).start()
        for d in range(NX):
            c_copy(ref, k, d).wait_recv()

    with jax.named_scope("gather_x"):
        gather_tp(xa, 0)

    @pl.loop(0, NL)
    def _(i):
        r = pl.ds(pl.multiple_of(i * NY * CAP, NY * CAP), NY * CAP)
        for x in range(NX):
            for c in range(NC):
                v = xa[x, c, i].astype(F32)
                col = (x * NC + c) * WCOL
                xr[r, col : col + 128] = v[:, :CAP].reshape(NY * CAP, 128).astype(BF)
                xr[r, col + 128 : col + 256] = v[:, CAP:].reshape(NY * CAP, 128).astype(BF)

    with jax.named_scope("w_zw"):
        wait_bytes(gw.at[0], loc.at[W])
        wait_bytes(gw.at[0:15], z_recv.at[W])
    outs[1].start()
    hid_rows = 128

    @pl.loop(0, ROWS // hid_rows)
    def _(i):
        r = pl.ds(pl.multiple_of(i * hid_rows, hid_rows), hid_rows)
        both = jnp.dot(xr[r, :], gw[...].reshape(WIDTH, 256), preferred_element_type=F32)
        v = both[:, 0:128]
        hh[mx, mc, r, :] = (v / (1.0 + jnp.exp(-v)) * both[:, 128:256]).astype(BF)

    with jax.named_scope("gather_h"):
        gather_tp(hh, 1)

    def back_dist(delta):
        if delta < 4:
            return -delta
        if delta > 4:
            return NL - delta
        return NL * (zl % 2) - 4


    def tp_copy(h, d):
        t = (tp + d) % NTP
        return copy_to(
            dw.at[h, pl.ds(t * 2, 2)], dn.at[tp, h], x_send.at[2 + h, d], x_recv.at[2 + h, d],
            {"x": t // NC, "c": t % NC},
        )

    def own_dn(h):
        return pltpu.make_async_copy(dw.at[h, pl.ds(tp * 2, 2)], dn.at[tp, h], loc.at[5 + h])

    def back(h, delta, ys):
        return copy_to(
            os_.at[h, (zl + NL - delta) % NL, ys], rt.at[h, my, zl], b_send.at[h, min(delta, 1)], b_recv.at[h],
            {**at_z(zz + back_dist(delta)), "y": ys},
        )

    def back_own(h):
        return pltpu.make_async_copy(os_.at[h, zl, my], rt.at[h, my, zl], b_recv.at[h])

    def give_back(h):
        with jax.named_scope("w_zd"):
            wait_bytes(dw.at[h, 0], loc.at[D + h])
            wait_bytes(dw.at[h, 0:15], z_recv.at[D + h])
        for delta in (4, 3, 5, 2, 6, 1, 7, 0):
            src_zl = (zl + NL - delta) % NL
            r = pl.ds(pl.multiple_of(src_zl * NY * CAP, NY * CAP), NY * CAP)
            acc = jnp.zeros((NY * CAP, 128), F32)
            for x in range(NX):
                lhs = jnp.concatenate([hh[x, 0, r, :], hh[x, 1, r, :]], axis=1)
                acc += jnp.dot(lhs, dw[h, 4 * x : 4 * x + 4].reshape(256, 128), preferred_element_type=F32)
            os_[h, src_zl] = acc.reshape(NY, 3, 8, 128).astype(BF)
            for d in range(NY):
                if delta or d:
                    back(h, delta, (my + d) % NY).start()
        back_own(h).start()
        own_dn(h).start()
        for d in (1, 7, 2, 6, 3, 5, 4):
            tp_copy(h, d).start()

    with jax.named_scope("give0"):
        give_back(0)
    with jax.named_scope("give1"):
        give_back(1)
    with jax.named_scope("w_back"):
        for h in range(2):
            wait_bytes(rt.at[h], b_recv.at[h])

    with jax.named_scope("drain"):
        for h in range(2):
            own_dn(h).wait()
            for d in range(1, NTP):
                tp_copy(h, d).wait()
            wait_bytes(dw.at[h, 0:15], z_send.at[D + h])
            wait_bytes(os_.at[h, 0, 0:3], b_send.at[h, 0])
            wait_bytes(os_.at[h, 0:7], b_send.at[h, 1])
        for copy in outs:
            copy.wait()
        for kind in (T, W, D):
            for d in (1, 3, 2):
                y_copy(kind, d).wait_send()
        wait_bytes(xa.at[0, 0, 0:7], z_send.at[T])
        wait_bytes(gw.at[0:15], z_send.at[W])
        for ref, k in ((xa, 0), (hh, 1)):
            for d in (1, 3, 2):
                x_copy(ref, k, d).wait_send()
            for d in range(NX):
                c_copy(ref, k, d).wait_send()


def finish(
    gw_in, dn_in, rt_in, cols_in, gate_out, up_out, down_out, mixed_out, gw, dn, rt, cols, rr, mixed, in_sem, sem
):
    ins = [
        pltpu.make_async_copy(far, near, in_sem.at[i])
        for i, (far, near) in enumerate(((cols_in, cols), (rt_in, rt), (gw_in, gw), (dn_in, dn)))
    ]
    for copy in ins:
        copy.start()
    place = lax.broadcasted_iota(jnp.int32, (TOK, ROWS), 1).astype(F32)
    ins[0].wait()
    q0 = (place == cols[:, 0:1]).astype(F32).astype(BF)
    q1 = (place == cols[:, 1:2]).astype(F32).astype(BF)

    ins[1].wait()
    for h in range(2):
        for yy in range(NY):
            r = slice(yy * NL * CAP, (yy + 1) * NL * CAP)
            rr[r, h * 128 : h * 128 + 128] = rt[h, yy].astype(F32).reshape(NL * CAP, 128).astype(BF)
    copies = []

    def put(near, far):
        copies.append(pltpu.make_async_copy(near, far, sem.at[len(copies)]))
        copies[-1].start()

    ins[2].wait()
    put(gw.at[:, :, :, 0:128], gate_out)
    put(gw.at[:, :, :, 128:256], up_out)
    ins[3].wait()
    for t in range(NTP):
        for h in range(2):
            at = t * WCOL + h * 128
            put(dn.at[t, h], down_out.at[:, :, :, at : at + 128])
    for i in range(TOK // 128):
        r = slice(i * 128, (i + 1) * 128)
        one = jnp.dot(q0[r, :], rr[...], preferred_element_type=F32)
        two = jnp.dot(q1[r, :], rr[...], preferred_element_type=F32)
        mixed[r, :] = (cols[r, 2:3] * one + cols[r, 3:4] * two).astype(BF)
        put(mixed.at[r], mixed_out.at[r])
    for copy in copies:
        copy.wait()


def local(tokens, route_ids, route_weights, norm_gain, gate_weight, up_weight, down_weight):
    hbm = pl.BlockSpec(memory_space=pltpu.HBM)
    free = pl.BlockSpec(memory_space=pl.ANY)
    dma = pltpu.SemaphoreType.DMA
    moved = pl.pallas_call(
        kernel,
        out_shape=(
            jax.ShapeDtypeStruct((NZ, NY, 32, 256), BF),
            jax.ShapeDtypeStruct((NTP, 2, 2, NY, 16, 128), BF),
            jax.ShapeDtypeStruct((2, NY, NL, 3, 8, 128), BF),
            jax.ShapeDtypeStruct((TOK, 128), F32),
        ),
        in_specs=[hbm] * 7,
        out_specs=(free,) * 4,
        scratch_shapes=[
            pltpu.VMEM((TOK, WIDTH), BF),
            pltpu.VMEM((2, TOK), jnp.int32),
            pltpu.VMEM((2, TOK), F32),
            pltpu.VMEM((1, 32), F32),
            pltpu.VMEM((EXP, 32, 128), F32),
            pltpu.VMEM((EXP, 32, 128), F32),
            pltpu.VMEM((EXP, 16, WCOL), F32),
            pltpu.VMEM((NY, NL, 32, 256), BF),
            pltpu.VMEM((NY, NL, 32, 256), BF),
            pltpu.VMEM((NZ, NY, 32, 256), BF),
            pltpu.VMEM((2, NY, NL, 16, 128), BF),
            pltpu.VMEM((2, NY, NL, 16, 128), BF),
            pltpu.VMEM((2, NZ, NY, 16, 128), BF),
            pltpu.VMEM((NY, NL, 2 * CAP, 128), BF),
            pltpu.VMEM((NY, NL, 2 * CAP, 128), BF),
            pltpu.VMEM((NX, NC, NL, NY, 2 * CAP, 128), BF),
            pltpu.VMEM((ROWS, WIDTH), BF),
            pltpu.VMEM((NX, NC, ROWS, 128), BF),
            pltpu.VMEM((2, NL, NY, 3, 8, 128), BF),
            pltpu.VMEM((TOK, WCOL), BF),
            pltpu.VMEM((TOK, 128), F32),
            dma((3, NY)),
            dma((3, NY)),
            dma((4,)),
            dma((4,)),
            dma((4, NTP)),
            dma((4, NTP)),
            dma((2, 2)),
            dma((2,)),
            dma((7,)),
            dma((7,)),
            dma((2,)),
            pltpu.SemaphoreType.REGULAR((2,)),
        ],
        compiler_params=pltpu.CompilerParams(
            collective_id=0, has_side_effects=True, vmem_limit_bytes=VMEM_MOVE * 1024 * 1024
        ),
        name="handoff",
    )(
        tokens,
        route_ids.T,
        route_weights.T,
        norm_gain.reshape(1, 32),
        gate_weight,
        up_weight,
        down_weight,
    )
    gate_new, up_new, down_new, mixed = pl.pallas_call(
        finish,
        out_shape=(
            jax.ShapeDtypeStruct((NZ, NY, 32, 128), BF),
            jax.ShapeDtypeStruct((NZ, NY, 32, 128), BF),
            jax.ShapeDtypeStruct((2, NY, 16, WIDTH), BF),
            jax.ShapeDtypeStruct((TOK, WCOL), BF),
        ),
        in_specs=[hbm] * 4,
        out_specs=(hbm,) * 4,
        scratch_shapes=[
            pltpu.VMEM((NZ, NY, 32, 256), BF),
            pltpu.VMEM((NTP, 2, 2, NY, 16, 128), BF),
            pltpu.VMEM((2, NY, NL, 3, 8, 128), BF),
            pltpu.VMEM((TOK, 128), F32),
            pltpu.VMEM((ROWS, WCOL), BF),
            pltpu.VMEM((TOK, WCOL), BF),
            dma((4,)),
            dma((2 + 2 * NTP + TOK // 128,)),
        ],
        compiler_params=pltpu.CompilerParams(vmem_limit_bytes=VMEM_LAST * 1024 * 1024),
        name="finish",
    )(*moved)
    return (
        gate_new.reshape(1, WIDTH, 128),
        up_new.reshape(1, WIDTH, 128),
        down_new.reshape(1, 128, WIDTH),
        mixed,
    )


def solution(mesh):
    torus = Mesh(mesh.devices.reshape(NH, NL, NY, NX, NC), ("zh", "zl", "y", "x", "c"))
    rows, cols = ("zh", "zl", "y"), ("x", "c")
    placed = (P(rows, None),) * 3 + (P(rows),) + (P(None, rows, cols),) * 3
    experts = ("zl", "y")
    return jax.shard_map(
        local,
        mesh=torus,
        in_specs=placed,
        out_specs=(P(experts, None, cols), P(experts, None, cols), P(experts, cols, None), P(rows, cols)),
        check_vma=False,
    )
```

```python
import jax
import jax.numpy as jnp
from jax import lax
from jax.experimental import pallas as pl
from jax.experimental.pallas import tpu as pltpu
from jax.sharding import Mesh
from jax.sharding import PartitionSpec as P

MESH = pl.DeviceIdType.MESH
BF, F32 = jnp.bfloat16, jnp.float32
NZ, NH, NL, NY, NX, NC = 16, 2, 8, 4, 4, 2
NTP = NX * NC
TOK, WIDTH, CAP, EXP = 384, 2048, 24, 32
WCOL = WIDTH // NTP
ROWS = EXP * CAP
NEAR, CUT = 4, 4
NG, GT = 4, TOK // 4
VMEM_MOVE, VMEM_LAST = 57, 57


def halves_down(v):
    return jnp.concatenate([v[:, :, :128], v[:, :, 128:]], axis=1)


def kernel(
    tokens_in, ids_in, wts_in, gain_in, gate_in, up_in, down_in,
    gw_out, dn, rt, cols_out,
    tokens, ids, wts, gain, gate, up, down, ws, yw, gw, ds, yd, dw, gs, gb, yt, xa, xr, hh, os_, rr, cols,
    y_send, y_recv, z_send, z_recv, x_send, x_recv, b_send, b_recv, loc, in_sem, out_sem, far_in, g_send, g_recv, t_send, t_recv, h_send, h_recv,
):
    zh, zl, my = lax.axis_index("zh"), lax.axis_index("zl"), lax.axis_index("y")
    mx, mc = lax.axis_index("x"), lax.axis_index("c")
    zz = zh * NL + zl
    tp = mx * NC + mc

    def at_z(z):
        z = (z + 2 * NZ) % NZ
        return {"zh": z // NL, "zl": z % NL}

    def copy_to(src, dst, send, recv, dev):
        return pltpu.make_async_remote_copy(
            src_ref=src, dst_ref=dst, send_sem=send, recv_sem=recv, device_id=dev, device_id_type=MESH
        )

    def wait_bytes(ref, sem):
        pltpu.make_async_copy(ref, ref, sem).wait()

    bar = pltpu.get_barrier_semaphore()

    def greet(dev):
        pl.semaphore_signal(bar, inc=1, device_id=dev, device_id_type=MESH)

    @pl.loop(0, NEAR)
    def _(i):
        greet(at_z(zz + NEAR - i))
        greet(at_z(zz + NZ - NEAR + i))

    ins = [
        pltpu.make_async_copy(far, near, in_sem.at[i])
        for i, (far, near) in enumerate(
            (
                (gate_in, gate), (up_in, up), (gain_in, gain), (tokens_in, tokens), (ids_in, ids), (wts_in, wts),
                (down_in, down),
            )
        )
    ]
    for copy in ins:
        copy.start()

    @pl.loop(1, NY)
    def _(d):
        greet({"y": (my + d) % NY})

    @pl.loop(1, NTP)
    def _(d):
        t = (tp + d) % NTP
        greet({"x": t // NC, "c": t % NC})

    with jax.named_scope("w_gain"):
        ins[2].wait()
        eye = lax.broadcasted_iota(jnp.int32, (32, 32), 0) == lax.broadcasted_iota(jnp.int32, (32, 32), 1)
    g = jnp.sum(jnp.where(eye, jnp.broadcast_to(gain[...], (32, 32)), 0.0), axis=1, keepdims=True)
    g = jnp.broadcast_to(g, (32, 128))
    with jax.named_scope("fold"):
        ins[0].wait()
        ins[1].wait()
        for yy in range(NY):
            for zt in range(NL):
                e = zt * NY + yy
                ws[yy, zt, :, 0:128] = (gate[e] * g).astype(BF)
                ws[yy, zt, :, 128:256] = (up[e] * g).astype(BF)

    with jax.named_scope("w_bar"):
        pl.semaphore_wait(bar, (NY - 1) + 2 * NEAR + (NTP - 1))
    for i, z in enumerate((zz + NEAR, zz + NZ - NEAR)):
        pl.semaphore_signal(far_in.at[i], inc=1, device_id=at_z(z), device_id_type=MESH)

    T, W, D = 0, 1, 2

    def y_copy(k, d):
        to = (my + d) % NY
        src, dst = (
            (yt.at[to], xa.at[mx, mc, :, my]) if k == T else (ws.at[to], yw.at[my]) if k == W else (ds.at[:, to], yd.at[:, my])
        )
        return copy_to(src, dst, y_send.at[k, d], y_recv.at[k, d], {"y": to})

    par = zl % 2
    toward = 1 - 2 * par

    def tok_src(i):
        return (zl + NL - i * toward) % NL

    def tok_send(i):
        j = (0, 3 - 2 * par, 1 + 2 * par, 2)[i]
        off = (0, 2 * par - 1, 2 - 4 * par, 6 * par - 3)[i]
        return copy_to(gs.at[(zl // 2 + j) % NG], gb.at[zl], g_send.at[0, i], g_recv.at[0, i], at_z(zz + off))

    def tok_relay(i):
        src = gb.at[tok_src(i)] if i else gs.at[zl // 2]
        return copy_to(src, gb.at[tok_src(i)], g_send.at[1, i], g_recv.at[1, i], at_z(zz + toward))

    own_group = pltpu.make_async_copy(gs.at[zl // 2], gb.at[zl], loc.at[7])

    def z_weights(src, into, k, ys):
        def send(far):
            copy_to(src.at[far % NL], into.at[zz, ys], z_send.at[k], z_recv.at[k], at_z(far)).start()

        send(zz + NL)

        @pl.loop(1, NL)
        def _(i):
            send(zz + NL + i)
            send(zz + NL - i)

        pltpu.make_async_copy(src.at[zl], into.at[zz, ys], loc.at[k]).start()

    def z_down(h):
        def send(far):
            copy_to(yd.at[h, :, far % NL], dw.at[h, zz], z_send.at[D + h], z_recv.at[D + h], at_z(far)).start()

        send(zz + NL)
        pltpu.make_async_copy(yd.at[h, :, zl], dw.at[h, zz], loc.at[D + h]).start()

        @pl.loop(1, NL)
        def _(i):
            send(zz + NL + i)
            send(zz + NL - i)

    def own_w(far):
        copy_to(ws.at[my, far % NL], gw.at[zz, my], z_send.at[W], z_recv.at[W], at_z(far)).start()

    with jax.named_scope("send_w"):
        for d in (1, 3, 2):
            y_copy(W, d).start()
        pltpu.make_async_copy(ws.at[my, zl], gw.at[zz, my], loc.at[W]).start()

        @pl.loop(0, NEAR)
        def _(i):
            own_w(zz + NEAR - i)
            own_w(zz + NZ - NEAR + i)

    def relabel(e):
        return (e % NY) * NL + e // NY

    ins[4].wait()
    ins[5].wait()
    first_r, second_r = relabel(ids[0:1, :]), relabel(ids[1:2, :])
    ex = lax.broadcasted_iota(jnp.int32, (EXP, TOK), 0)
    member_r = (ex == first_r) | (ex == second_r)
    a = lax.broadcasted_iota(jnp.int32, (TOK, TOK), 0)
    b = lax.broadcasted_iota(jnp.int32, (TOK, TOK), 1)
    before = (a < b).astype(F32).astype(BF)
    rank_r = jnp.dot(member_r.astype(F32).astype(BF), before, preferred_element_type=F32)
    rank_r = jnp.where(member_r, rank_r, -1.0)

    ins[3].wait()

    @pl.loop(0, TOK // 64)
    def _(i):
        r = pl.ds(pl.multiple_of(i * 64, 64), 64)
        v = tokens[r, :].astype(F32)
        scale = lax.rsqrt(jnp.mean(v * v, axis=-1, keepdims=True) + 1e-06)
        own = pl.ds(pl.multiple_of(tp * WCOL, WCOL), WCOL)
        rr[r, :] = (tokens[r, own].astype(F32) * scale).astype(BF)

    mine = rr[0:TOK, :]
    slots = [jnp.sum(jnp.where(ex == e_k, rank_r, 0.0), axis=0, keepdims=True) for e_k in (first_r, second_r)]
    group = ids[0:1, :] // NL
    in_group = lax.broadcasted_iota(jnp.int32, (8, TOK), 0) == group
    place_r = jnp.dot(in_group.astype(F32).astype(BF), before, preferred_element_type=F32)
    place_r = jnp.sum(jnp.where(in_group, place_r, 0.0), axis=0, keepdims=True)
    spots = [(ids[k : k + 1, :] % NL).astype(F32) * CAP + slots[k] for k in range(2)]
    spots = jnp.concatenate([*spots, jnp.zeros((6, TOK), F32)], axis=0).astype(BF)
    row = lax.broadcasted_iota(jnp.int32, (128, TOK), 0).astype(F32)
    for g in range(NG):
        pick = ((row == place_r) & (group == g)).astype(F32).astype(BF)
        got = jnp.dot(pick, mine, preferred_element_type=F32)[:GT]
        gs[g, 0:12] = got[:, :128].reshape(12, 8, 128).astype(BF)
        gs[g, 12:24] = got[:, 128:].reshape(12, 8, 128).astype(BF)
        told = lax.dot_general(spots, pick, (((1,), (1,)), ((), ())), preferred_element_type=F32)
        gs[g, 24] = told.astype(BF)

    with jax.named_scope("send_t"):
        for i in (3, 2, 1):
            tok_send(i).start()
        own_group.start()
        tok_relay(0).start()

    with jax.named_scope("w_far"):
        pl.semaphore_wait(far_in.at[0], 1)
        pl.semaphore_wait(far_in.at[1], 1)
        own_w(zz + NL)

        @pl.loop(1, NL - NEAR)
        def _(i):
            own_w(zz + NL + i)
            own_w(zz + NL - i)

    ins[6].wait()
    for yy in range(NY):
        for zt in range(NL):
            both = down[zt * NY + yy].astype(BF)
            ds[0, yy, zt] = both[:, 0:128]
            ds[1, yy, zt] = both[:, 128:256]

    for d in (1, 3, 2):
        y_copy(D, d).start()
    own_down = pltpu.make_async_copy(ds.at[:, my], yd.at[:, my], loc.at[4])
    own_down.start()
    def send_others(ds, first=0, last=NL):
        def send(far):
            for d in ds:
                ys = (my + NY - d) % NY
                copy_to(yw.at[ys, far % NL], gw.at[zz, ys], z_send.at[W], z_recv.at[W], at_z(far)).start()

        if first == 0:
            for d in ds:
                y_copy(W, d).wait_recv()
                ys = (my + NY - d) % NY
                pltpu.make_async_copy(yw.at[ys, zl], gw.at[zz, ys], loc.at[W]).start()
            send(zz + NL)

        @pl.loop(max(first, 1), last)
        def _(i):
            send(zz + NL + i)
            send(zz + NL - i)

    with jax.named_scope("fwd_w1"):
        send_others((1,), 0, CUT)
    with jax.named_scope("fwd_t"):
        for i in (1, 2, 3):
            tok_send(i).wait_recv()
            tok_relay(i).start()
    with jax.named_scope("fwd_w"):
        send_others((1,), CUT, NL)
        send_others((3, 2))
    with jax.named_scope("fwd_d"):
        for d in (1, 3, 2):
            y_copy(D, d).wait_recv()
        own_down.wait()
        z_down(0)
        z_down(1)


    with jax.named_scope("w_grp"):
        own_group.wait()
        for i in range(4):
            tok_relay(i).wait_recv()
    want = (lax.broadcasted_iota(jnp.int32, (NY * CAP, 128), 0) + par * (NY * CAP)).astype(F32)

    @pl.loop(0, NL)
    def _(i):
        v = gb[i].astype(F32)
        told = v[24]
        pick = ((want == told[0:1, :]) | (want == told[1:2, :])).astype(F32).astype(BF)
        body = jnp.concatenate([v[0:12].reshape(GT, 128), v[12:24].reshape(GT, 128)], axis=1)
        body = jnp.concatenate([body, jnp.zeros((128 - GT, WCOL), F32)], axis=0).astype(BF)
        got = halves_down(jnp.dot(pick, body, preferred_element_type=F32).reshape(NY, CAP, WCOL)).astype(BF)
        for yy in range(NY):
            yt[yy, i] = got[yy]

    for d in (1, 3, 2):
        y_copy(T, d).start()
    own_tok = pltpu.make_async_copy(yt.at[my], xa.at[mx, mc, :, my], loc.at[T])
    own_tok.start()

    def x_tok(n, d):
        ys = (my + NY - (0, 1, 3, 2)[n]) % NY
        rows = xa.at[mx, mc, :, ys]
        return copy_to(rows if n else yt.at[my], rows, t_send.at[n, d], t_recv.at[n, d], {"x": (mx + d) % NX})

    for d in (1, 3, 2):
        x_tok(0, d).start()

    ats = [slots[k] + e_k.astype(F32) * CAP for k, e_k in enumerate((first_r, second_r))]
    turned = jnp.concatenate([*ats, wts[...], jnp.zeros((4, TOK), F32)], axis=0).T
    cols[...] = jnp.concatenate([turned, jnp.zeros((TOK, 120), F32)], axis=1)
    outs = [
        pltpu.make_async_copy(near, far, out_sem.at[i])
        for i, (near, far) in enumerate(((cols, cols_out), (gw, gw_out)))
    ]
    outs[0].start()

    with jax.named_scope("w_ztok"):
        for n, d in ((1, 1), (2, 3), (3, 2)):
            y_copy(T, d).wait_recv()
            for to in (1, 3, 2):
                x_tok(n, to).start()
        own_tok.wait()

    def c_copy(ref, k, d):
        who = (mx + NX - d) % NX
        return copy_to(
            ref.at[who, mc], ref.at[who, mc], x_send.at[k, NX + d], x_recv.at[k, NX + d], {"c": 1 - mc}
        )

    with jax.named_scope("gather_x"):
        c_copy(xa, 0, 0).start()
        for d in (1, 3, 2):
            for n in range(NY):
                x_tok(n, d).wait_recv()
            c_copy(xa, 0, d).start()
        for d in range(NX):
            c_copy(xa, 0, d).wait_recv()

    @pl.loop(0, NL)
    def _(i):
        r = pl.ds(pl.multiple_of(i * NY * CAP, NY * CAP), NY * CAP)
        for x in range(NX):
            for c in range(NC):
                v = xa[x, c, i].astype(F32)
                col = (x * NC + c) * WCOL
                xr[r, col : col + 128] = v[:, :CAP].reshape(NY * CAP, 128).astype(BF)
                xr[r, col + 128 : col + 256] = v[:, CAP:].reshape(NY * CAP, 128).astype(BF)

    with jax.named_scope("w_zw"):
        wait_bytes(gw.at[0], loc.at[W])
        wait_bytes(gw.at[0:15], z_recv.at[W])
    outs[1].start()
    hid_rows = ROWS // 4

    def x_hid(n, d):
        at = hh.at[mx, mc, n * hid_rows : (n + 1) * hid_rows]
        return copy_to(at, at, h_send.at[n, d], h_recv.at[n, d], {"x": (mx + d) % NX})

    def c_hid(n, d):
        at = hh.at[(mx + NX - d) % NX, mc, n * hid_rows : (n + 1) * hid_rows]
        return copy_to(at, at, h_send.at[n, NX + d], h_recv.at[n, NX + d], {"c": 1 - mc})

    for n in range(4):
        r = slice(n * hid_rows, (n + 1) * hid_rows)
        both = jnp.dot(xr[r, :], gw[...].reshape(WIDTH, 256), preferred_element_type=F32)
        v = both[:, 0:128]
        hh[mx, mc, r, :] = (v / (1.0 + jnp.exp(-v)) * both[:, 128:256]).astype(BF)
        for d in (2, 1, 3):
            x_hid(n, d).start()
        c_hid(n, 0).start()

    with jax.named_scope("gather_h"):
        for n in range(4):
            for d in (1, 3, 2):
                x_hid(n, d).wait_recv()
                c_hid(n, d).start()
        for n in range(4):
            for d in range(NX):
                c_hid(n, d).wait_recv()

    def back_dist(delta):
        if delta < 4:
            return -delta
        if delta > 4:
            return NL - delta
        return 4 - NL * (zl % 2)


    def tp_copy(h, d):
        t = (tp + d) % NTP
        return copy_to(
            dw.at[h, pl.ds(t * 2, 2)], dn.at[tp, h], x_send.at[2 + h, d], x_recv.at[2 + h, d],
            {"x": t // NC, "c": t % NC},
        )

    def own_dn(h):
        return pltpu.make_async_copy(dw.at[h, pl.ds(tp * 2, 2)], dn.at[tp, h], loc.at[5 + h])

    def back(h, delta, ys):
        return copy_to(
            os_.at[h, (zl + NL - delta) % NL, ys], rt.at[h, my, zl], b_send.at[h, min(delta, 1)], b_recv.at[h],
            {**at_z(zz + back_dist(delta)), "y": ys},
        )

    def back_own(h):
        return pltpu.make_async_copy(os_.at[h, zl, my], rt.at[h, my, zl], b_recv.at[h])

    def give_back(h):
        with jax.named_scope("w_zd"):
            wait_bytes(dw.at[h, 0], loc.at[D + h])
            wait_bytes(dw.at[h, 0:15], z_recv.at[D + h])
        for delta in (4, 3, 5, 2, 6, 1, 7, 0):
            src_zl = (zl + NL - delta) % NL
            r = pl.ds(pl.multiple_of(src_zl * NY * CAP, NY * CAP), NY * CAP)
            acc = jnp.zeros((NY * CAP, 128), F32)
            for x in range(NX):
                lhs = jnp.concatenate([hh[x, 0, r, :], hh[x, 1, r, :]], axis=1)
                acc += jnp.dot(lhs, dw[h, 4 * x : 4 * x + 4].reshape(256, 128), preferred_element_type=F32)
            os_[h, src_zl] = acc.reshape(NY, 3, 8, 128).astype(BF)
            for d in range(NY):
                if delta or d:
                    back(h, delta, (my + d) % NY).start()
        back_own(h).start()
        own_dn(h).start()
        for d in (1, 7, 2, 6, 3, 5, 4):
            tp_copy(h, d).start()

    with jax.named_scope("give0"):
        give_back(0)
    with jax.named_scope("give1"):
        give_back(1)
    with jax.named_scope("w_back"):
        for h in range(2):
            wait_bytes(rt.at[h], b_recv.at[h])

    with jax.named_scope("drain"):
        for h in range(2):
            own_dn(h).wait()
            for d in range(1, NTP):
                tp_copy(h, d).wait()
            wait_bytes(dw.at[h, 0:15], z_send.at[D + h])
            wait_bytes(os_.at[h, 0, 0:3], b_send.at[h, 0])
            wait_bytes(os_.at[h, 0:7], b_send.at[h, 1])
        for copy in outs:
            copy.wait()
        for kind in (T, W, D):
            for d in (1, 3, 2):
                y_copy(kind, d).wait_send()
        for i in range(4):
            if i:
                tok_send(i).wait_send()
            tok_relay(i).wait_send()
        wait_bytes(gw.at[0:15], z_send.at[W])
        for d in (1, 3, 2):
            for n in range(4):
                x_hid(n, d).wait_send()
                x_tok(n, d).wait_send()
        for d in range(NX):
            c_copy(xa, 0, d).wait_send()
            for n in range(4):
                c_hid(n, d).wait_send()


def finish(
    gw_in, dn_in, rt_in, cols_in, gate_out, up_out, down_out, mixed_out, gw, dn, rt, cols, rr, mixed, in_sem, sem
):
    ins = [
        pltpu.make_async_copy(far, near, in_sem.at[i])
        for i, (far, near) in enumerate(((cols_in, cols), (rt_in, rt), (gw_in, gw), (dn_in, dn)))
    ]
    for copy in ins:
        copy.start()
    place = lax.broadcasted_iota(jnp.int32, (TOK, ROWS), 1).astype(F32)
    ins[0].wait()
    q0 = (place == cols[:, 0:1]).astype(F32).astype(BF)
    q1 = (place == cols[:, 1:2]).astype(F32).astype(BF)

    ins[1].wait()
    for h in range(2):
        for yy in range(NY):
            r = slice(yy * NL * CAP, (yy + 1) * NL * CAP)
            rr[r, h * 128 : h * 128 + 128] = rt[h, yy].astype(F32).reshape(NL * CAP, 128).astype(BF)
    copies = []

    def put(near, far):
        copies.append(pltpu.make_async_copy(near, far, sem.at[len(copies)]))
        copies[-1].start()

    ins[2].wait()
    put(gw.at[:, :, :, 0:128], gate_out)
    put(gw.at[:, :, :, 128:256], up_out)
    ins[3].wait()
    for t in range(NTP):
        for h in range(2):
            at = t * WCOL + h * 128
            put(dn.at[t, h], down_out.at[:, :, :, at : at + 128])
    for i in range(TOK // 128):
        r = slice(i * 128, (i + 1) * 128)
        one = jnp.dot(q0[r, :], rr[...], preferred_element_type=F32)
        two = jnp.dot(q1[r, :], rr[...], preferred_element_type=F32)
        mixed[r, :] = (cols[r, 2:3] * one + cols[r, 3:4] * two).astype(BF)
        put(mixed.at[r], mixed_out.at[r])
    for copy in copies:
        copy.wait()


def local(tokens, route_ids, route_weights, norm_gain, gate_weight, up_weight, down_weight):
    hbm = pl.BlockSpec(memory_space=pltpu.HBM)
    free = pl.BlockSpec(memory_space=pl.ANY)
    dma = pltpu.SemaphoreType.DMA
    moved = pl.pallas_call(
        kernel,
        out_shape=(
            jax.ShapeDtypeStruct((NZ, NY, 32, 256), BF),
            jax.ShapeDtypeStruct((NTP, 2, 2, NY, 16, 128), BF),
            jax.ShapeDtypeStruct((2, NY, NL, 3, 8, 128), BF),
            jax.ShapeDtypeStruct((TOK, 128), F32),
        ),
        in_specs=[hbm] * 7,
        out_specs=(free,) * 4,
        scratch_shapes=[
            pltpu.VMEM((TOK, WIDTH), BF),
            pltpu.VMEM((2, TOK), jnp.int32),
            pltpu.VMEM((2, TOK), F32),
            pltpu.VMEM((1, 32), F32),
            pltpu.VMEM((EXP, 32, 128), F32),
            pltpu.VMEM((EXP, 32, 128), F32),
            pltpu.VMEM((EXP, 16, WCOL), F32),
            pltpu.VMEM((NY, NL, 32, 256), BF),
            pltpu.VMEM((NY, NL, 32, 256), BF),
            pltpu.VMEM((NZ, NY, 32, 256), BF),
            pltpu.VMEM((2, NY, NL, 16, 128), BF),
            pltpu.VMEM((2, NY, NL, 16, 128), BF),
            pltpu.VMEM((2, NZ, NY, 16, 128), BF),
            pltpu.VMEM((NG, GT // 4 + 1, 8, 128), BF),
            pltpu.VMEM((NL, GT // 4 + 1, 8, 128), BF),
            pltpu.VMEM((NY, NL, 2 * CAP, 128), BF),
            pltpu.VMEM((NX, NC, NL, NY, 2 * CAP, 128), BF),
            pltpu.VMEM((ROWS, WIDTH), BF),
            pltpu.VMEM((NX, NC, ROWS, 128), BF),
            pltpu.VMEM((2, NL, NY, 3, 8, 128), BF),
            pltpu.VMEM((TOK, WCOL), BF),
            pltpu.VMEM((TOK, 128), F32),
            dma((3, NY)),
            dma((3, NY)),
            dma((4,)),
            dma((4,)),
            dma((4, NTP)),
            dma((4, NTP)),
            dma((2, 2)),
            dma((2,)),
            dma((8,)),
            dma((7,)),
            dma((2,)),
            pltpu.SemaphoreType.REGULAR((2,)),
            dma((2, 4)),
            dma((2, 4)),
            dma((NY, NX)),
            dma((NY, NX)),
            dma((4, 2 * NX)),
            dma((4, 2 * NX)),
        ],
        compiler_params=pltpu.CompilerParams(
            collective_id=0, has_side_effects=True, vmem_limit_bytes=VMEM_MOVE * 1024 * 1024
        ),
        name="handoff",
    )(
        tokens,
        route_ids.T,
        route_weights.T,
        norm_gain.reshape(1, 32),
        gate_weight,
        up_weight,
        down_weight,
    )
    gate_new, up_new, down_new, mixed = pl.pallas_call(
        finish,
        out_shape=(
            jax.ShapeDtypeStruct((NZ, NY, 32, 128), BF),
            jax.ShapeDtypeStruct((NZ, NY, 32, 128), BF),
            jax.ShapeDtypeStruct((2, NY, 16, WIDTH), BF),
            jax.ShapeDtypeStruct((TOK, WCOL), BF),
        ),
        in_specs=[hbm] * 4,
        out_specs=(hbm,) * 4,
        scratch_shapes=[
            pltpu.VMEM((NZ, NY, 32, 256), BF),
            pltpu.VMEM((NTP, 2, 2, NY, 16, 128), BF),
            pltpu.VMEM((2, NY, NL, 3, 8, 128), BF),
            pltpu.VMEM((TOK, 128), F32),
            pltpu.VMEM((ROWS, WCOL), BF),
            pltpu.VMEM((TOK, WCOL), BF),
            dma((4,)),
            dma((2 + 2 * NTP + TOK // 128,)),
        ],
        compiler_params=pltpu.CompilerParams(vmem_limit_bytes=VMEM_LAST * 1024 * 1024),
        name="finish",
    )(*moved)
    return (
        gate_new.reshape(1, WIDTH, 128),
        up_new.reshape(1, WIDTH, 128),
        down_new.reshape(1, 128, WIDTH),
        mixed,
    )


def solution(mesh):
    torus = Mesh(mesh.devices.reshape(NH, NL, NY, NX, NC), ("zh", "zl", "y", "x", "c"))
    rows, cols = ("zh", "zl", "y"), ("x", "c")
    placed = (P(rows, None),) * 3 + (P(rows),) + (P(None, rows, cols),) * 3
    experts = ("zl", "y")
    return jax.shard_map(
        local,
        mesh=torus,
        in_specs=placed,
        out_specs=(P(experts, None, cols), P(experts, None, cols), P(experts, cols, None), P(rows, cols)),
        check_vma=False,
    )
```
